32 devices in a mesh: sp: 8 (over z, y), tp: 4 (over x, core).
Axes of the slice: x: 2, y: 2, z: 4, core: 2. Of those that a mesh axis runs over, the one named last changes fastest.
Arguments:
- tokens: bfloat16 [4, 4096, 2048], P(None, ('sp', 'tp')), may hold values from -6 to 6
- in_gain: float32 [2048], replicated, may hold values from 0.1 to 1.9
- query_weight: bfloat16 [2048, 1024], P(None, 'tp'), may hold values from -0.125 to 0.125
- key_weight: bfloat16 [2048, 1024], P(None, 'tp'), may hold values from -0.125 to 0.125
- value_weight: bfloat16 [2048, 1024], P(None, 'tp'), may hold values from -0.125 to 0.125
- gate_weight: bfloat16 [2048, 1024], P(None, 'tp'), may hold values from -0.125 to 0.125
- log_decay: float32 [8], P('tp'), may hold values from -0.034 to 0, as said below
- norm_gain: float32 [1024], P('tp'), may hold values from 0.1 to 1.9
- out_weight: bfloat16 [1024, 2048], replicated, may hold values from -0.1875 to 0.1875
- post_gain: float32 [2048], replicated, may hold values from 0.1 to 1.9
Outputs:
- mixed: bfloat16 [4, 4096, 2048], P(None, ('sp', 'tp'))
The draws below stay inside these ranges and needn't reach their ends.
Inputs may be any that keep to these rules, and one draw needn't show every extreme that they name: `log_decay`: every entry is negative; some heads keep a tenth or more of their memory over 4096 positions, others lose most of it within 30 to 100 positions.
All inputs are finite; a program needn't handle non-finite values.
Results may differ from the reference program's by a relative error of at most 0.015.
Values may be sent and summed in bfloat16 or wider, within the bound.
A program may use at most 64 MiB of HBM per device.

```python
import math
import jax
import jax.numpy as jnp
from jax import lax

D = 2048
HEADS = 8
HEAD_DIM = 128
BLOCK = 128
SEQS = 4
RET_WIDTH = 1024
SEQLEN = 4096


def draw_log_decay(key, part):
    head_order = jax.random.permutation(jax.random.fold_in(key, 11), HEADS)
    slow_heads = head_order < HEADS // 2
    uniform_draw = jax.random.uniform(jax.random.fold_in(key, 12), (HEADS,), jnp.float32)
    slow_rate = math.log(10.0) / SEQLEN * (0.1 + 0.9 * uniform_draw)
    fast_rate = jnp.exp(math.log(1.0 / 100.0) + uniform_draw * (math.log(1.0 / 30.0) - math.log(1.0 / 100.0)))
    return -jnp.where(slow_heads, slow_rate, fast_rate).astype(jnp.float32)


def level_of(stream_key, dims, pieces, smallest, high):
    level = 1.0
    for position, parts in pieces:
        steps = jax.random.uniform(jax.random.fold_in(jax.random.fold_in(stream_key, 6), position), (parts,), jnp.float32, smallest / len(pieces), high / len(pieces))
        level = level * jnp.repeat(jnp.exp(steps), dims[position] // parts).reshape((-1,) + (1,) * (len(dims) - 1 - position))
    return level


def noise(own_key, shape, scale, reach, split=(), kind=jnp.bfloat16):
    level = level_of(own_key, shape, split, -0.22, 0.18) if split else 1.0
    values = jax.random.normal(own_key, shape, jnp.float32) * scale * level
    return jnp.minimum(jnp.maximum(values, -reach), reach).astype(kind)


def setup_inputs(seed: int = 0) -> dict:
    keys = jax.random.split(jax.random.key(seed), 11)
    return {
        "tokens": noise(keys[0], (SEQS, SEQLEN, D), 1.0, 6.0, ((1, 32),)),
        "in_gain": jnp.clip(1.0 + 0.18 * jax.random.normal(keys[1], (D,), jnp.float32), 0.1, 1.9),
        "query_weight": noise(keys[2], (D, RET_WIDTH), D ** -0.5, 0.125, ((1, 4),)),
        "key_weight": noise(keys[3], (D, RET_WIDTH), D ** -0.5, 0.125, ((1, 4),)),
        "value_weight": noise(keys[4], (D, RET_WIDTH), D ** -0.5, 0.125, ((1, 4),)),
        "gate_weight": noise(keys[5], (D, RET_WIDTH), D ** -0.5, 0.125, ((1, 4),)),
        "log_decay": draw_log_decay(jax.random.fold_in(keys[10], 71), 0),
        "norm_gain": jnp.clip(1.0 + 0.18 * jax.random.normal(keys[7], (RET_WIDTH,), jnp.float32), 0.1, 1.9),
        "out_weight": noise(keys[8], (RET_WIDTH, D), RET_WIDTH ** -0.5, 0.1875),
        "post_gain": jnp.clip(1.0 + 0.18 * jax.random.normal(keys[9], (D,), jnp.float32), 0.1, 1.9),
    }


rms_eps = 1e-06
group_eps = 1e-05
rope_base = 10000.0
highest = lax.Precision.HIGHEST

def rotate(values, positions):
    half_dim = values.shape[-1] // 2
    inverse = rope_base ** (-jnp.arange(half_dim, dtype=jnp.float32) / half_dim)
    angles = positions.astype(jnp.float32)[:, None] * inverse[None, :]
    cosine = jnp.cos(angles)
    sine_part = jnp.sin(angles)
    first_half = values[..., :half_dim].astype(jnp.float32)
    second = values[..., half_dim:].astype(jnp.float32)
    return jnp.concatenate([first_half * cosine - second * sine_part, first_half * sine_part + second * cosine], axis=-1)

def retain(queries, key_rows, values, log_decay):
    seq_count, head_count, length, head_width = queries.shape
    block_count = length // BLOCK
    offsets = jnp.arange(BLOCK, dtype=jnp.float32)
    distance = offsets[:, None] - offsets[None, :]
    rate_col = log_decay[:, None, None]
    inside = jnp.where(distance >= 0, jnp.exp(rate_col * jnp.maximum(distance, 0.0)), 0.0)
    query_scale = jnp.exp(log_decay[:, None] * (offsets + 1.0))[..., None]
    key_scale = jnp.exp(log_decay[:, None] * (BLOCK - 1.0 - offsets))[..., None]
    block_decay = jnp.exp(log_decay * BLOCK)[:, None, None]

    def to_blocks(arr):
        return arr.reshape(seq_count, head_count, block_count, BLOCK, arr.shape[-1]).transpose(2, 0, 1, 3, 4)

    def advance(memory, inputs):
        q_block, k_block, v_block = inputs
        qf = q_block.astype(jnp.float32)
        kf = k_block.astype(jnp.float32)
        vf = v_block.astype(jnp.float32)
        scores = jnp.einsum('shqd,shkd->shqk', qf, kf, precision=highest)
        weights = (scores * inside).astype(jnp.bfloat16)
        within = jnp.einsum('shqk,shkv->shqv', weights.astype(jnp.float32), vf, precision=highest)
        carried = jnp.einsum('shqd,shdv->shqv', qf * query_scale, memory, precision=highest)
        k_scaled = (kf * key_scale).astype(jnp.bfloat16)
        memory = memory * block_decay + jnp.einsum('shkd,shkv->shdv', k_scaled.astype(jnp.float32), vf, precision=highest)
        return (memory, within + carried)
    start_memory = jnp.zeros((seq_count, head_count, head_width, values.shape[-1]), jnp.float32)
    outputs = lax.scan(advance, start_memory, (to_blocks(queries), to_blocks(key_rows), to_blocks(values)))[1]
    return outputs.transpose(1, 2, 0, 3, 4).reshape(seq_count, head_count, length, values.shape[-1])

def reference(tokens, in_gain, query_weight, key_weight, value_weight, gate_weight, log_decay, norm_gain, out_weight, post_gain):
    seq_count, length, model_width = tokens.shape
    tok_f32 = tokens.astype(jnp.float32)
    normed = (tok_f32 * lax.rsqrt(lax.optimization_barrier(jnp.mean(tok_f32 * tok_f32, axis=-1, keepdims=True)) + rms_eps) * in_gain).astype(jnp.bfloat16)
    flat_rows = normed.reshape(seq_count * length, model_width)

    def project(weight_mat):
        result = jnp.dot(flat_rows, weight_mat, preferred_element_type=jnp.float32).astype(jnp.bfloat16)
        return result.reshape(seq_count, length, HEADS, HEAD_DIM).transpose(0, 2, 1, 3)
    positions = jnp.arange(length, dtype=jnp.int32)
    queries = rotate(project(query_weight), positions).astype(jnp.bfloat16)
    key_rows = (rotate(project(key_weight), positions) * HEAD_DIM ** (-0.5)).astype(jnp.bfloat16)
    values = project(value_weight)
    gating = jnp.dot(flat_rows, gate_weight, preferred_element_type=jnp.float32).astype(jnp.bfloat16)
    gating = gating.reshape(seq_count, length, RET_WIDTH)
    retained = retain(queries, key_rows, values, log_decay)
    center = lax.optimization_barrier(jnp.mean(retained, axis=-1, keepdims=True))
    spread = lax.optimization_barrier(jnp.mean(jnp.square(retained - center), axis=-1, keepdims=True))
    normal = ((retained - center) * lax.rsqrt(spread + group_eps)).transpose(0, 2, 1, 3).reshape(seq_count, length, RET_WIDTH)
    gated = (normal * norm_gain * jax.nn.silu(gating.astype(jnp.float32))).astype(jnp.bfloat16)
    premix = jnp.dot(gated.reshape(seq_count * length, RET_WIDTH), out_weight, preferred_element_type=jnp.float32)
    mixed = premix * lax.rsqrt(lax.optimization_barrier(jnp.mean(premix * premix, axis=-1, keepdims=True)) + rms_eps) * post_gain
    return mixed.astype(jnp.bfloat16).reshape(seq_count, length, model_width)
```

```python
import functools
import math

import jax
import jax.numpy as jnp
import numpy as np
from jax import lax
from jax.experimental import pallas as pl
from jax.experimental.pallas import tpu as pltpu
from jax.sharding import PartitionSpec as P

HEAD_DIM = 128
SUB = 128
rms_eps = 1e-06
group_eps = 1e-05
rope_base = 10000.0
MESH = pl.DeviceIdType.MESH
F32 = jnp.float32
BF16 = jnp.bfloat16


def kernel(
    tp, sp,
    tok, gain, wq_h, wk_h, wv_h, wg_h, decay, ngain, wo_h, pgain, inv,
    out,
    gath, wq, wk, wv, wg, wo, nb, cosv, sinv, mask, qs, ks, vs, gs,
    within, state, excl, st_out, st_in, g_out, g_in, premix,
    x_send, p_send, t_recv, s_send, s_recv, g_send, g_recv, w_sem, own_sem,
):
    seqs, rows, width = tok.shape
    length = rows * tp
    cols = wq.shape[1]
    heads = cols // HEAD_DIM
    chips = tp // 2
    pair = 2 * rows
    rounds = [1 << k for k in range(max(1, (sp - 1).bit_length()))] if sp > 1 else []
    last = len(rounds) - 1
    s, t = lax.axis_index("sp"), lax.axis_index("tp")
    chip, core = lax.div(t, 2), lax.rem(t, 2)
    other = chip * 2 + 1 - core

    barrier = pltpu.get_barrier_semaphore()
    for j in range(1, tp):
        pl.semaphore_signal(
            barrier, inc=1, device_id={"tp": lax.rem(t + j, tp)}, device_id_type=MESH
        )
    for d in rounds:
        @pl.when(s + d < sp)
        def _():
            pl.semaphore_signal(barrier, inc=1, device_id={"sp": s + d}, device_id_type=MESH)

        @pl.when(s >= d)
        def _():
            pl.semaphore_signal(barrier, inc=1, device_id={"sp": s - d}, device_id_type=MESH)

    peers = jnp.int32(tp - 1)
    for d in rounds:
        peers = peers + jnp.where(s + d < sp, 1, 0) + jnp.where(s >= d, 1, 0)
    pl.semaphore_wait(barrier, peers)

    def block(q, who):
        return gath.at[q, pl.ds(pl.multiple_of(who * rows, rows), rows), :]

    def to_chip(q, j):
        peer = lax.rem(chip + j, chips) * 2 + core
        return pltpu.make_async_remote_copy(
            tok.at[q], block(q, t), x_send.at[q, j], t_recv.at[q, t],
            device_id={"tp": peer}, device_id_type=MESH,
        )

    def to_core(q, who, mine):
        return pltpu.make_async_remote_copy(
            tok.at[q] if mine else block(q, who), block(q, who),
            p_send.at[q, who], t_recv.at[q, who],
            device_id={"tp": other}, device_id_type=MESH,
        )

    def arrived(q, who):
        pltpu.make_async_remote_copy(
            tok.at[q], block(q, who), p_send.at[q, who], t_recv.at[q, who],
            device_id={"tp": other}, device_id_type=MESH,
        ).wait_recv()

    for q in range(seqs):
        for j in range(1, chips):
            to_chip(q, j).start()
    own = [pltpu.make_async_copy(tok.at[q], block(q, t), own_sem.at[q]) for q in range(seqs)]
    for q in range(seqs):
        own[q].start()
        to_core(q, t, True).start()
    loads = [
        pltpu.make_async_copy(a, b, w_sem.at[i])
        for i, (a, b) in enumerate(
            ((wq_h, wq), (wk_h, wk), (wv_h, wv), (wg_h, wg), (wo_h, wo))
        )
    ]
    for load in loads:
        load.start()

    place = (s * length + lax.broadcasted_iota(jnp.int32, (length, HEAD_DIM), 0)).astype(F32)
    angle = place * inv[...]
    cosv[...] = jnp.cos(angle)
    lane = lax.broadcasted_iota(jnp.int32, (length, HEAD_DIM), 1)
    sine = jnp.sin(angle)
    sinv[...] = jnp.where(lane < HEAD_DIM // 2, -sine, sine)
    for h in range(heads):
        def fill(i, _):
            at = pl.multiple_of(i * 32, 32)
            gap = (
                at + lax.broadcasted_iota(jnp.int32, (32, length), 0)
                - lax.broadcasted_iota(jnp.int32, (32, length), 1)
            )
            weight = jnp.exp(decay[h] * jnp.maximum(gap, 0).astype(F32))
            mask[h, pl.ds(at, 32), :] = jnp.where(gap >= 0, weight, 0.0)
            return 0

        lax.fori_loop(0, length // 32, fill, 0)
    excl[...] = jnp.zeros_like(excl)

    def head(h):
        return slice(h * HEAD_DIM, (h + 1) * HEAD_DIM)

    def project(q, which):
        base = pl.multiple_of(which * pair, pair)

        def norm(i, _):
            at = pl.multiple_of(i * 16, 16)
            x = gath[q, pl.ds(pl.multiple_of(base + at, 16), 16), :].astype(F32)
            scale = lax.rsqrt(jnp.mean(x * x, axis=-1, keepdims=True) + rms_eps)
            nb[pl.ds(at, 16), :] = (x * scale * gain[...]).astype(BF16)
            return 0

        lax.fori_loop(0, pair // 16, norm, 0)
        span = pl.ds(base, pair)
        for w, dest, kind in ((wk, ks, 2), (wv, vs, 0), (wq, qs, 1), (wg, gs, 0)):
            r = jnp.dot(nb[...], w[...], preferred_element_type=F32).astype(BF16)
            if kind == 0:
                dest[q, span, :] = r
            else:
                for h in range(heads):
                    x = r[:, head(h)].astype(F32)
                    x = x * cosv[span, :] + pltpu.roll(x, HEAD_DIM // 2, 1) * sinv[span, :]
                    if kind == 2:
                        x = x * HEAD_DIM ** (-0.5)
                    dest[q, span, head(h)] = x.astype(BF16)

    def send_state(q, k):
        for h in range(heads):
            total = state[q, h] + jnp.exp(jnp.full((1, 1), decay[h] * length, F32)) * excl[q, h]
            st_out[q, k, h] = total.astype(BF16)

        @pl.when(s + rounds[k] < sp)
        def _():
            state_copy(q, k).start()

    def state_copy(q, k):
        return pltpu.make_async_remote_copy(
            st_out.at[q, k], st_in.at[q, k], s_send.at[q, k], s_recv.at[q, k],
            device_id={"sp": lax.rem(s + rounds[k], sp)}, device_id_type=MESH,
        )

    def take_state(q, k):
        @pl.when(s >= rounds[k])
        def _():
            state_copy(q, k).wait_recv()
            for h in range(heads):
                rate = jnp.exp(jnp.full((1, 1), decay[h] * (length * (rounds[k] - 1)), F32))
                excl[q, h] += rate * st_in[q, k, h].astype(F32)

    def make_state(q):
        spot = lax.broadcasted_iota(jnp.int32, (length, HEAD_DIM), 0)
        for h in range(heads):
            fade = jnp.exp(decay[h] * (length - 1 - spot).astype(F32))
            scaled = (ks[q, :, head(h)].astype(F32) * fade).astype(BF16)
            state[q, h] = lax.dot_general(
                scaled, vs[q, :, head(h)], (((0,), (0,)), ((), ())), preferred_element_type=F32
            )

    def inside(q):
        for h in range(heads):
            for i in range(length // SUB):
                here, upto = slice(i * SUB, (i + 1) * SUB), slice(0, (i + 1) * SUB)
                score = lax.dot_general(
                    qs[q, here, head(h)], ks[q, upto, head(h)],
                    (((1,), (1,)), ((), ())), preferred_element_type=F32,
                )
                weight = (score * mask[h, here, upto]).astype(BF16)
                within[q, here, head(h)] = jnp.dot(
                    weight, vs[q, upto, head(h)], preferred_element_type=F32
                )

    def gated_copy(q, j):
        dest = lax.rem(t + j, tp)
        return pltpu.make_async_remote_copy(
            g_out.at[q, pl.ds(pl.multiple_of(dest * rows, rows), rows), :],
            g_in.at[q, :, pl.ds(pl.multiple_of(t * cols, cols), cols)],
            g_send.at[q, j], g_recv.at[q, j],
            device_id={"tp": dest}, device_id_type=MESH,
        )

    def gated_own(q):
        return pltpu.make_async_copy(
            g_out.at[q, pl.ds(pl.multiple_of(t * rows, rows), rows), :],
            g_in.at[q, :, pl.ds(pl.multiple_of(t * cols, cols), cols)],
            g_recv.at[q, 0],
        )

    def finish(q):
        for h in range(heads):
            memory = excl[q, h].astype(BF16)
            for i in range(length // SUB):
                here = slice(i * SUB, (i + 1) * SUB)
                spot = i * SUB + 1 + lax.broadcasted_iota(jnp.int32, (SUB, HEAD_DIM), 0)
                reach = jnp.exp(decay[h] * spot.astype(F32))
                query = (qs[q, here, head(h)].astype(F32) * reach).astype(BF16)
                kept = within[q, here, head(h)] + jnp.dot(
                    query, memory, preferred_element_type=F32
                )
                kept = kept - jnp.mean(kept, axis=-1, keepdims=True)
                spread = jnp.mean(kept * kept, axis=-1, keepdims=True)
                normal = kept * lax.rsqrt(spread + group_eps) * ngain[:, head(h)]
                gate = gs[q, here, head(h)].astype(F32)
                g_out[q, here, head(h)] = (normal * (gate * jax.nn.sigmoid(gate))).astype(BF16)
        for j in range(1, tp):
            gated_copy(q, j).start()
        gated_own(q).start()

    def emit(q):
        for j in range(1, tp):
            gated_copy(q, j).wait_recv()
        gated_own(q).wait()
        step = min(512, width)
        for c in range(width // step):
            part = slice(c * step, (c + 1) * step)
            premix[:, part] = jnp.dot(g_in[q], wo[:, part], preferred_element_type=F32)

        def norm(i, _):
            at = pl.multiple_of(i * 16, 16)
            x = premix[pl.ds(at, 16), :]
            scale = lax.rsqrt(jnp.mean(x * x, axis=-1, keepdims=True) + rms_eps)
            out[q, pl.ds(at, 16), :] = (x * scale * pgain[...]).astype(BF16)
            return 0

        lax.fori_loop(0, rows // 16, norm, 0)

    for q in range(seqs):
        own[q].wait()
    for load in loads:
        load.wait()

    def near(q, _):
        arrived(q, other)
        project(q, chip)
        return 0

    lax.fori_loop(0, seqs, near, 0)

    def far(q, _):
        for j in range(1, chips):
            who = lax.rem(chip + j, chips)
            mine, theirs = who * 2 + core, who * 2 + 1 - core
            arrived(q, mine)
            to_core(q, mine, False).start()
        if last > 0:
            @pl.when(q > 0)
            def _():
                for k in range(1, last):
                    take_state(q - 1, k)
                    send_state(q - 1, k + 1)
        for j in range(1, chips):
            who = lax.rem(chip + j, chips)
            arrived(q, who * 2 + 1 - core)
            project(q, who)
        make_state(q)
        if rounds:
            send_state(q, 0)
        inside(q)

        @pl.when(q > 0)
        def _():
            if last >= 0:
                take_state(q - 1, last)
            finish(q - 1)

        if last > 0:
            take_state(q, 0)
            send_state(q, 1)
        return 0

    lax.fori_loop(0, seqs, far, 0)

    end = seqs - 1
    if last > 0:
        for k in range(1, last):
            take_state(end, k)
            send_state(end, k + 1)
    if last >= 0:
        take_state(end, last)
    finish(end)

    def write(q, _):
        emit(q)
        return 0

    lax.fori_loop(0, seqs, write, 0)

    def drain(q, _):
        for j in range(1, chips):
            to_chip(q, j).wait_send()
            to_core(q, lax.rem(chip + j, chips) * 2 + core, False).wait_send()
        to_core(q, t, True).wait_send()
        for j in range(1, tp):
            gated_copy(q, j).wait_send()
        for k, d in enumerate(rounds):
            @pl.when(s + d < sp)
            def _():
                state_copy(q, k).wait_send()
        return 0

    lax.fori_loop(0, seqs, drain, 0)


def solution(mesh):
    tp, sp = mesh.shape["tp"], mesh.shape["sp"]

    def body(tok, gain, wq, wk, wv, wg, decay, ngain, wo, pgain):
        seqs, rows, width = tok.shape
        cols = wq.shape[1]
        heads = cols // HEAD_DIM
        length = rows * tp
        half = HEAD_DIM // 2
        inv = rope_base ** (-jnp.arange(half, dtype=F32) / half)
        inv = jnp.concatenate([inv, inv])[None, :]
        steps = max(1, (sp - 1).bit_length())
        dma = pltpu.SemaphoreType.DMA
        any_, vmem = pl.BlockSpec(memory_space=pl.ANY), pl.BlockSpec(memory_space=pltpu.VMEM)
        wide = pltpu.VMEM((seqs, length, cols), BF16)
        return pl.pallas_call(
            functools.partial(kernel, tp, sp),
            out_shape=jax.ShapeDtypeStruct(tok.shape, BF16),
            in_specs=[
                any_, vmem, any_, any_, any_, any_,
                pl.BlockSpec(memory_space=pltpu.SMEM), vmem, any_, vmem, vmem,
            ],
            out_specs=vmem,
            scratch_shapes=[
                pltpu.VMEM((seqs, length, width), BF16),
                pltpu.VMEM(wq.shape, BF16), pltpu.VMEM(wq.shape, BF16),
                pltpu.VMEM(wq.shape, BF16), pltpu.VMEM(wq.shape, BF16),
                pltpu.VMEM(wo.shape, BF16),
                pltpu.VMEM((2 * rows, width), BF16),
                pltpu.VMEM((length, HEAD_DIM), F32), pltpu.VMEM((length, HEAD_DIM), F32),
                pltpu.VMEM((heads, length, length), F32),
                wide, wide, wide, wide,
                pltpu.VMEM((seqs, length, cols), F32),
                pltpu.VMEM((seqs, heads, HEAD_DIM, HEAD_DIM), F32),
                pltpu.VMEM((seqs, heads, HEAD_DIM, HEAD_DIM), F32),
                pltpu.VMEM((seqs, steps, heads, HEAD_DIM, HEAD_DIM), BF16),
                pltpu.VMEM((seqs, steps, heads, HEAD_DIM, HEAD_DIM), BF16),
                wide,
                pltpu.VMEM((seqs, rows, cols * tp), BF16),
                pltpu.VMEM((rows, width), F32),
                dma((seqs, max(2, tp // 2))), dma((seqs, tp)), dma((seqs, tp)),
                dma((seqs, steps)), dma((seqs, steps)),
                dma((seqs, tp)), dma((seqs, tp)),
                dma((5,)), dma((seqs,)),
            ],
            compiler_params=pltpu.CompilerParams(
                collective_id=0, has_side_effects=True, vmem_limit_bytes=60 * 2**20
            ),
            name="retention",
        )(
            tok, gain[None, :], wq, wk, wv, wg, decay, ngain[None, :], wo, pgain[None, :], inv
        )

    placed = (
        P(None, ("sp", "tp"), None),
        P(),
        P(None, "tp"),
        P(None, "tp"),
        P(None, "tp"),
        P(None, "tp"),
        P("tp"),
        P("tp"),
        P(),
        P(),
    )
    return jax.shard_map(
        body, mesh=mesh, in_specs=placed, out_specs=P(None, ("sp", "tp"), None), check_vma=False
    )
```

```python
import functools
import math

import jax
import jax.numpy as jnp
import numpy as np
from jax import lax
from jax.experimental import pallas as pl
from jax.experimental.pallas import tpu as pltpu
from jax.sharding import PartitionSpec as P

HEAD_DIM = 128
SUB = 128
rms_eps = 1e-06
group_eps = 1e-05
rope_base = 10000.0
MESH = pl.DeviceIdType.MESH
F32 = jnp.float32
BF16 = jnp.bfloat16


def kernel(
    tp, sp,
    tok, gain_h, wq_h, wk_h, wv_h, wg_h, decay, ngain_h, wo_h, pgain_h, inv_h,
    out,
    gain, ngain, pgain, inv, gath, wq, wk, wv, wg, wo, nb, cosv, sinv, mask, qs, ks, vs, gs,
    within, state, excl, st_out, st_in, g_out, g_in, premix,
    x_send, p_send, t_recv, s_send, s_recv, g_send, g_recv, w_sem, own_sem,
):
    seqs, rows, width = tok.shape
    length = rows * tp
    cols = wq.shape[1]
    heads = cols // HEAD_DIM
    chips = tp // 2
    pair = 2 * rows
    rounds = [1 << k for k in range(max(1, (sp - 1).bit_length()))] if sp > 1 else []
    last = len(rounds) - 1
    s, t = lax.axis_index("sp"), lax.axis_index("tp")
    chip, core = lax.div(t, 2), lax.rem(t, 2)
    other = chip * 2 + 1 - core

    barrier = pltpu.get_barrier_semaphore()
    for j in range(1, tp):
        pl.semaphore_signal(
            barrier, inc=1, device_id={"tp": lax.rem(t + j, tp)}, device_id_type=MESH
        )
    for d in rounds:
        @pl.when(s + d < sp)
        def _():
            pl.semaphore_signal(barrier, inc=1, device_id={"sp": s + d}, device_id_type=MESH)

        @pl.when(s >= d)
        def _():
            pl.semaphore_signal(barrier, inc=1, device_id={"sp": s - d}, device_id_type=MESH)

    peers = jnp.int32(tp - 1)
    for d in rounds:
        peers = peers + jnp.where(s + d < sp, 1, 0) + jnp.where(s >= d, 1, 0)
    pl.semaphore_wait(barrier, peers)

    def block(q, who):
        return gath.at[q, pl.ds(pl.multiple_of(who * rows, rows), rows), :]

    def to_chip(q, j):
        peer = lax.rem(chip + j, chips) * 2 + core
        return pltpu.make_async_remote_copy(
            tok.at[q], block(q, t), x_send.at[q, j], t_recv.at[q, t],
            device_id={"tp": peer}, device_id_type=MESH,
        )

    def to_core(q, who, mine):
        return pltpu.make_async_remote_copy(
            tok.at[q] if mine else block(q, who), block(q, who),
            p_send.at[q, who], t_recv.at[q, who],
            device_id={"tp": other}, device_id_type=MESH,
        )

    def arrived(q, who):
        pltpu.make_async_remote_copy(
            tok.at[q], block(q, who), p_send.at[q, who], t_recv.at[q, who],
            device_id={"tp": other}, device_id_type=MESH,
        ).wait_recv()

    for q in range(seqs):
        for j in range(1, chips):
            to_chip(q, j).start()
    own = [pltpu.make_async_copy(tok.at[q], block(q, t), own_sem.at[q]) for q in range(seqs)]
    for q in range(seqs):
        own[q].start()
        to_core(q, t, True).start()
    loads = [
        pltpu.make_async_copy(a, b, w_sem.at[i])
        for i, (a, b) in enumerate(
            (
                (inv_h, inv), (gain_h, gain), (ngain_h, ngain), (pgain_h, pgain),
                (wk_h, wk), (wv_h, wv), (wq_h, wq), (wg_h, wg), (wo_h, wo),
            )
        )
    ]
    for load in loads:
        load.start()

    loads[0].wait()
    place = (s * length + lax.broadcasted_iota(jnp.int32, (length, HEAD_DIM), 0)).astype(F32)
    angle = place * inv[...]
    cosv[...] = jnp.cos(angle)
    lane = lax.broadcasted_iota(jnp.int32, (length, HEAD_DIM), 1)
    sine = jnp.sin(angle)
    sinv[...] = jnp.where(lane < HEAD_DIM // 2, -sine, sine)
    for h in range(heads):
        def fill(i, _):
            at = pl.multiple_of(i * 32, 32)
            gap = (
                at + lax.broadcasted_iota(jnp.int32, (32, length), 0)
                - lax.broadcasted_iota(jnp.int32, (32, length), 1)
            )
            weight = jnp.exp(decay[h] * jnp.maximum(gap, 0).astype(F32))
            mask[h, pl.ds(at, 32), :] = jnp.where(gap >= 0, weight, 0.0)
            return 0

        lax.fori_loop(0, length // 32, fill, 0)
    excl[...] = jnp.zeros_like(excl)

    def head(h):
        return slice(h * HEAD_DIM, (h + 1) * HEAD_DIM)

    def normalise(q, who):
        base = pl.multiple_of(who * rows, rows)

        def norm(i, _):
            at = pl.multiple_of(base + i * 16, 16)
            x = gath[q, pl.ds(at, 16), :].astype(F32)
            scale = lax.rsqrt(jnp.mean(x * x, axis=-1, keepdims=True) + rms_eps)
            nb[pl.ds(at, 16), :] = (x * scale * gain[...]).astype(BF16)
            return 0

        lax.fori_loop(0, rows // 16, norm, 0, unroll=2)

    def project(q, which, parts):
        span = pl.ds(pl.multiple_of(which * pair, pair), pair)
        for w, dest, kind in parts:
            r = jnp.dot(nb[span, :], w[...], preferred_element_type=F32).astype(BF16)
            if kind == 0:
                dest[q, span, :] = r
            else:
                for h in range(heads):
                    x = r[:, head(h)].astype(F32)
                    x = x * cosv[span, :] + pltpu.roll(x, HEAD_DIM // 2, 1) * sinv[span, :]
                    if kind == 2:
                        x = x * HEAD_DIM ** (-0.5)
                    dest[q, span, head(h)] = x.astype(BF16)

    first = ((wk, ks, 2), (wv, vs, 0))
    second = ((wq, qs, 1), (wg, gs, 0))

    def send_state(q, k):
        for h in range(heads):
            total = state[q, h] + jnp.exp(jnp.full((1, 1), decay[h] * length, F32)) * excl[q, h]
            st_out[q, k, h] = total.astype(BF16)

        @pl.when(s + rounds[k] < sp)
        def _():
            state_copy(q, k).start()

    def state_copy(q, k):
        return pltpu.make_async_remote_copy(
            st_out.at[q, k], st_in.at[q, k], s_send.at[q, k], s_recv.at[q, k],
            device_id={"sp": lax.rem(s + rounds[k], sp)}, device_id_type=MESH,
        )

    def take_state(q, k):
        @pl.when(s >= rounds[k])
        def _():
            state_copy(q, k).wait_recv()
            for h in range(heads):
                rate = jnp.exp(jnp.full((1, 1), decay[h] * (length * (rounds[k] - 1)), F32))
                excl[q, h] += rate * st_in[q, k, h].astype(F32)

    def make_state(q):
        spot = lax.broadcasted_iota(jnp.int32, (length, HEAD_DIM), 0)
        for h in range(heads):
            fade = jnp.exp(decay[h] * (length - 1 - spot).astype(F32))
            scaled = (ks[q, :, head(h)].astype(F32) * fade).astype(BF16)
            state[q, h] = lax.dot_general(
                scaled, vs[q, :, head(h)], (((0,), (0,)), ((), ())), preferred_element_type=F32
            )

    def inside(q):
        for h in range(heads):
            for i in range(length // SUB):
                here, upto = slice(i * SUB, (i + 1) * SUB), slice(0, (i + 1) * SUB)
                score = lax.dot_general(
                    qs[q, here, head(h)], ks[q, upto, head(h)],
                    (((1,), (1,)), ((), ())), preferred_element_type=F32,
                )
                weight = (score * mask[h, here, upto]).astype(BF16)
                within[q, here, head(h)] = jnp.dot(
                    weight, vs[q, upto, head(h)], preferred_element_type=F32
                )

    def gated_copy(q, dest, source):
        return pltpu.make_async_remote_copy(
            g_out.at[q, pl.ds(pl.multiple_of(dest * rows, rows), rows), :],
            g_in.at[q, :, pl.ds(pl.multiple_of(source * cols, cols), cols)],
            g_send.at[q, dest], g_recv.at[q, source],
            device_id={"tp": dest}, device_id_type=MESH,
        )

    def gated_own(q):
        return pltpu.make_async_copy(
            g_out.at[q, pl.ds(pl.multiple_of(t * rows, rows), rows), :],
            g_in.at[q, :, pl.ds(pl.multiple_of(t * cols, cols), cols)],
            g_recv.at[q, t],
        )

    def members(j):
        base = lax.rem(chip + j, chips) * 2
        return base + core, base + 1 - core

    def finish(q):
        for dest in [d for j in range(1, chips) for d in members(j)] + [other, t]:
            here = pl.ds(pl.multiple_of(dest * rows, rows), rows)
            spot = dest * rows + 1 + lax.broadcasted_iota(jnp.int32, (rows, HEAD_DIM), 0)
            for h in range(heads):
                reach = jnp.exp(decay[h] * spot.astype(F32))
                query = (qs[q, here, head(h)].astype(F32) * reach).astype(BF16)
                kept = within[q, here, head(h)] + jnp.dot(
                    query, excl[q, h].astype(BF16), preferred_element_type=F32
                )
                kept = kept - jnp.mean(kept, axis=-1, keepdims=True)
                spread = jnp.mean(kept * kept, axis=-1, keepdims=True)
                normal = kept * lax.rsqrt(spread + group_eps) * ngain[:, head(h)]
                gate = gs[q, here, head(h)].astype(F32)
                g_out[q, here, head(h)] = (normal * (gate * jax.nn.sigmoid(gate))).astype(BF16)
            if dest is t:
                gated_own(q).start()
            else:
                gated_copy(q, dest, t).start()

    def emit(q):
        step = min(512, width)
        for j in range(chips):
            if j == 0:
                gated_own(q).wait()
                gated_copy(q, other, other).wait_recv()
            else:
                for source in members(j):
                    gated_copy(q, other, source).wait_recv()
            span = pl.ds(pl.multiple_of(lax.rem(chip + j, chips) * 2 * cols, 2 * cols), 2 * cols)
            for c in range(width // step):
                part = slice(c * step, (c + 1) * step)
                term = jnp.dot(g_in[q, :, span], wo[span, part], preferred_element_type=F32)
                premix[:, part] = term if j == 0 else premix[:, part] + term

        def norm(i, _):
            at = pl.multiple_of(i * 16, 16)
            x = premix[pl.ds(at, 16), :]
            scale = lax.rsqrt(jnp.mean(x * x, axis=-1, keepdims=True) + rms_eps)
            out[q, pl.ds(at, 16), :] = (x * scale * pgain[...]).astype(BF16)
            return 0

        lax.fori_loop(0, rows // 16, norm, 0, unroll=2)

    for q in range(seqs):
        own[q].wait()
    for load in loads[1:]:
        load.wait()

    def near(q, _):
        normalise(q, t)
        arrived(q, other)
        normalise(q, other)
        project(q, chip, first + second)
        return 0

    lax.fori_loop(0, seqs, near, 0)

    def far(q, _):
        for j in range(1, chips):
            mine, _ = members(j)
            arrived(q, mine)
            to_core(q, mine, False).start()
        if last > 0:
            @pl.when(q > 0)
            def _():
                for k in range(1, last):
                    take_state(q - 1, k)
                    send_state(q - 1, k + 1)
        for j in range(1, chips):
            mine, theirs = members(j)
            normalise(q, mine)
            arrived(q, theirs)
            normalise(q, theirs)
            project(q, lax.rem(chip + j, chips), first)
        make_state(q)
        if rounds:
            send_state(q, 0)
        for j in range(1, chips):
            project(q, lax.rem(chip + j, chips), second)
        if last > 0:
            take_state(q, 0)
            send_state(q, 1)
        inside(q)

        @pl.when(q > 0)
        def _():
            if last >= 0:
                take_state(q - 1, last)
            finish(q - 1)
        return 0

    lax.fori_loop(0, seqs, far, 0)

    def write(q, _):
        emit(q)
        return 0

    end = seqs - 1
    for k in range(1, last):
        take_state(end, k)
        send_state(end, k + 1)
    done = min(2, end)
    lax.fori_loop(0, done, write, 0)
    if last >= 0:
        take_state(end, last)
    finish(end)

    lax.fori_loop(done, seqs, write, 0)

    def drain(q, _):
        for j in range(1, chips):
            to_chip(q, j).wait_send()
            to_core(q, lax.rem(chip + j, chips) * 2 + core, False).wait_send()
        to_core(q, t, True).wait_send()
        for j in range(1, tp):
            gated_copy(q, lax.rem(t + j, tp), t).wait_send()
        for k, d in enumerate(rounds):
            @pl.when(s + d < sp)
            def _():
                state_copy(q, k).wait_send()
        return 0

    lax.fori_loop(0, seqs, drain, 0)


def solution(mesh):
    tp, sp = mesh.shape["tp"], mesh.shape["sp"]

    def body(tok, gain, wq, wk, wv, wg, decay, ngain, wo, pgain):
        seqs, rows, width = tok.shape
        cols = wq.shape[1]
        heads = cols // HEAD_DIM
        length = rows * tp
        half = HEAD_DIM // 2
        inv = np.float32(rope_base) ** (-np.arange(half, dtype=np.float32) / half)
        inv = jnp.asarray(np.concatenate([inv, inv])[None, :], F32)
        steps = max(1, (sp - 1).bit_length())
        dma = pltpu.SemaphoreType.DMA
        hbm, vmem = pl.BlockSpec(memory_space=pltpu.HBM), pl.BlockSpec(memory_space=pltpu.VMEM)
        wide = pltpu.VMEM((seqs, length, cols), BF16)
        return pl.pallas_call(
            functools.partial(kernel, tp, sp),
            out_shape=jax.ShapeDtypeStruct(tok.shape, BF16),
            in_specs=[
                hbm, hbm, hbm, hbm, hbm, hbm,
                pl.BlockSpec(memory_space=pltpu.SMEM), hbm, hbm, hbm, hbm,
            ],
            out_specs=vmem,
            scratch_shapes=[
                pltpu.VMEM((1, width), F32), pltpu.VMEM((1, cols), F32),
                pltpu.VMEM((1, width), F32), pltpu.VMEM((1, HEAD_DIM), F32),
                pltpu.VMEM((seqs, length, width), BF16),
                pltpu.VMEM(wq.shape, BF16), pltpu.VMEM(wq.shape, BF16),
                pltpu.VMEM(wq.shape, BF16), pltpu.VMEM(wq.shape, BF16),
                pltpu.VMEM(wo.shape, BF16),
                pltpu.VMEM((length, width), BF16),
                pltpu.VMEM((length, HEAD_DIM), F32), pltpu.VMEM((length, HEAD_DIM), F32),
                pltpu.VMEM((heads, length, length), F32),
                wide, wide, wide, wide,
                pltpu.VMEM((seqs, length, cols), F32),
                pltpu.VMEM((seqs, heads, HEAD_DIM, HEAD_DIM), F32),
                pltpu.VMEM((seqs, heads, HEAD_DIM, HEAD_DIM), F32),
                pltpu.VMEM((seqs, steps, heads, HEAD_DIM, HEAD_DIM), BF16),
                pltpu.VMEM((seqs, steps, heads, HEAD_DIM, HEAD_DIM), BF16),
                wide,
                pltpu.VMEM((seqs, rows, cols * tp), BF16),
                pltpu.VMEM((rows, width), F32),
                dma((seqs, max(2, tp // 2))), dma((seqs, tp)), dma((seqs, tp)),
                dma((seqs, steps)), dma((seqs, steps)),
                dma((seqs, tp)), dma((seqs, tp)),
                dma((9,)), dma((seqs,)),
            ],
            compiler_params=pltpu.CompilerParams(
                collective_id=0, has_side_effects=True, vmem_limit_bytes=59 * 2**20
            ),
            name="retention",
        )(
            tok, gain[None, :], wq, wk, wv, wg, decay, ngain[None, :], wo, pgain[None, :], inv
        )

    placed = (
        P(None, ("sp", "tp"), None),
        P(),
        P(None, "tp"),
        P(None, "tp"),
        P(None, "tp"),
        P(None, "tp"),
        P("tp"),
        P("tp"),
        P(),
        P(),
    )
    return jax.shard_map(
        body, mesh=mesh, in_specs=placed, out_specs=P(None, ("sp", "tp"), None), check_vma=False
    )
```
